32 devices in a mesh: fs: 8 (over z, y), tp: 4 (over x, core).
Axes of the slice: x: 2, y: 2, z: 4, core: 2. Of those that a mesh axis runs over, the one named last changes fastest.
Arguments:
- inputs: bfloat16 [2048, 2048], P('fs', 'tp'), may hold values from -6 to 6
- cotangent: bfloat16 [2048, 2048], P('fs', 'tp'), may hold values from -8 to 8
- gate_weight: bfloat16 [2048, 5632], P('fs', 'tp'), may hold values from -0.125 to 0.125
- up_weight: bfloat16 [2048, 5632], P('fs', 'tp'), may hold values from -0.125 to 0.125
- down_weight: bfloat16 [5632, 2048], P('tp', 'fs'), may hold values from -0.078125 to 0.078125
Outputs:
- grad_inputs: bfloat16 [2048, 2048], P('fs', 'tp')
- grad_gate: float32 [2048, 5632], P('fs', 'tp')
- grad_up: float32 [2048, 5632], P('fs', 'tp')
- grad_down: float32 [5632, 2048], P('tp', 'fs')
The draws below stay inside these ranges and needn't reach their ends.
All inputs are finite; a program needn't handle non-finite values.
Results may differ from the reference program's by a relative error of at most 0.015.
Values may be sent and summed in bfloat16 or wider, within the bound.
A program may use at most 64 MiB of HBM per device.

```python
import jax
import jax.numpy as jnp
from jax import lax

D = 2048
FF = 5632
TOKENS = 2048
N_TP = 4


def spiked(entries, own_key, source, target, blocks, factor):
    def block_of(axis_at):
        return (jnp.arange(entries.shape[axis_at]) // (entries.shape[axis_at] // blocks)).reshape((-1,) + (1,) * (entries.ndim - 1 - axis_at))

    near = jax.random.permutation(own_key, blocks)[block_of(target)]
    other_side = (block_of(target) + blocks // 2) % blocks
    return jnp.where((block_of(source) == near) | (block_of(source) == other_side), factor * entries, entries)


def levels(key, dims, cuts, smallest, high):
    level = 1.0
    for dim, blocks in cuts:
        steps = jax.random.uniform(jax.random.fold_in(jax.random.fold_in(key, 6), dim), (blocks,), jnp.float32, smallest / len(cuts), high / len(cuts))
        level = level * jnp.repeat(jnp.exp(steps), dims[dim] // blocks).reshape((-1,) + (1,) * (len(dims) - 1 - dim))
    return level


def scatter_about(own_key, extent, scale, most, split=(), kind=jnp.bfloat16):
    result = jax.random.normal(own_key, extent, jnp.float32) * scale
    if len(split) > 0:
        result = levels(own_key, extent, split, -0.22, 0.18) * result
    return jnp.clip(result, min=-most, max=most).astype(kind)


def heavy_noise(rng, shape, scale, bound, pieces, heavy, kind=jnp.bfloat16):
    entries = scale * jax.random.normal(rng, shape, jnp.float32)
    if pieces:
        entries = entries * levels(rng, shape, pieces, -0.22, 0.18)
    return jnp.clip(spiked(entries, jax.random.fold_in(rng, 3), *heavy), -bound, bound).astype(kind)


def setup_inputs(seed: int = 0) -> dict:
    keys = jax.random.split(jax.random.key(seed), 6)
    inputs = scatter_about(keys[0], (TOKENS, D), 1.0, 6.0, ((0, 8), (1, 4)))
    cotangent = heavy_noise(keys[1], (TOKENS, D), 1.0, 8.0, ((0, 8), (1, 4)), (0, 1, 8, 2.0))
    gate_weight = scatter_about(keys[2], (D, FF), D ** -0.5, 0.125, ((0, 8), (1, 4)))
    up_weight = scatter_about(keys[3], (D, FF), D ** -0.5, 0.125, ((0, 8), (1, 4)))
    down_weight = scatter_about(keys[4], (FF, D), FF ** -0.5, 0.078125, ((0, 4), (1, 8)))
    return {"inputs": inputs, "cotangent": cotangent, "gate_weight": gate_weight, "up_weight": up_weight, "down_weight": down_weight}


def contract_rows(left, right):
    return lax.dot_general(left, right, (((0,), (0,)), ((), ())), preferred_element_type=jnp.float32)


def contract_cols(left, right):
    return lax.dot_general(left, right, (((1,), (1,)), ((), ())), preferred_element_type=jnp.float32)


def reference(inputs, cotangent, gate_weight, up_weight, down_weight):
    gate_pre = jnp.dot(inputs, gate_weight, preferred_element_type=jnp.float32)
    up_pre = jnp.dot(inputs, up_weight, preferred_element_type=jnp.float32)
    gate_sig = jax.nn.sigmoid(gate_pre)
    gate_act = gate_pre * gate_sig
    hidden = (gate_act * up_pre).astype(jnp.bfloat16)
    grad_hidden = contract_cols(cotangent, down_weight)
    grad_gate_pre = (grad_hidden * up_pre * gate_sig * (1.0 + gate_pre * (1.0 - gate_sig))).astype(jnp.bfloat16)
    grad_up_pre = (grad_hidden * gate_act).astype(jnp.bfloat16)
    grad_gate = contract_rows(inputs, grad_gate_pre)
    grad_up = contract_rows(inputs, grad_up_pre)
    grad_down = contract_rows(hidden, cotangent)
    width = FF // N_TP

    def add_block(block_index, running):
        offset = (block_index * width).astype(jnp.int32)
        block_gate = lax.dynamic_slice_in_dim(grad_gate_pre, offset, width, 1)
        block_up = lax.dynamic_slice_in_dim(grad_up_pre, offset, width, 1)
        weight_gate = lax.dynamic_slice_in_dim(gate_weight, offset, width, 1)
        weight_up = lax.dynamic_slice_in_dim(up_weight, offset, width, 1)
        partial_sum = contract_cols(block_gate, weight_gate) + contract_cols(block_up, weight_up)
        rounded = lax.optimization_barrier(partial_sum.astype(jnp.bfloat16))
        return running + rounded.astype(jnp.float32)

    summed = lax.fori_loop(0, N_TP, add_block, jnp.zeros(inputs.shape, jnp.float32))
    grad_inputs = summed.astype(jnp.bfloat16)
    return (grad_inputs, grad_gate, grad_up, grad_down)
```

```python
import functools

import jax
import jax.numpy as jnp
from jax import lax
from jax.experimental import pallas as pl
from jax.experimental.pallas import tpu as pltpu
from jax.sharding import PartitionSpec as P

MESH = pl.DeviceIdType.MESH
ANY = pl.BlockSpec(memory_space=pl.ANY)
VMEM = pl.BlockSpec(memory_space=pltpu.VMEM)
CORES = 2


def contract_rows(left, right):
    return lax.dot_general(
        left, right, (((0,), (0,)), ((), ())), preferred_element_type=jnp.float32
    )


def contract_cols(left, right):
    return lax.dot_general(
        left, right, (((1,), (1,)), ((), ())), preferred_element_type=jnp.float32
    )


def gathered_plan(inputs, cotangent, gate_weight, up_weight, down_weight):
    whole_inputs = lax.all_gather(inputs, "tp", axis=1, tiled=True)
    whole_cotangent = lax.all_gather(cotangent, "tp", axis=1, tiled=True)
    gate_whole = lax.all_gather(gate_weight, "fs", axis=0, tiled=True)
    up_whole = lax.all_gather(up_weight, "fs", axis=0, tiled=True)
    down_whole = lax.all_gather(down_weight, "fs", axis=1, tiled=True)
    gate_pre = jnp.dot(whole_inputs, gate_whole, preferred_element_type=jnp.float32)
    up_pre = jnp.dot(whole_inputs, up_whole, preferred_element_type=jnp.float32)
    grad_hidden = contract_cols(whole_cotangent, down_whole)
    hidden, grad_gate_pre, grad_up_pre = pointwise(gate_pre, up_pre, grad_hidden)
    pre_grads = jnp.concatenate([grad_gate_pre, grad_up_pre], axis=1)
    width = gate_weight.shape[1]
    partial_sum = contract_cols(grad_gate_pre, gate_whole) + contract_cols(grad_up_pre, up_whole)

    def scattered(values, axis, dim):
        return lax.psum_scatter(
            values.astype(jnp.bfloat16), axis, scatter_dimension=dim, tiled=True
        )

    grad_inputs = scattered(partial_sum, "tp", 1)
    expand = scattered(contract_rows(whole_inputs, pre_grads), "fs", 0).astype(jnp.float32)
    down = scattered(contract_rows(whole_cotangent, hidden), "fs", 0).astype(jnp.float32)
    return (grad_inputs, expand[:, :width], expand[:, width:], down.T)


def pointwise(gate_pre, up_pre, grad_hidden):
    gate_sig = jax.nn.sigmoid(gate_pre)
    gate_act = gate_pre * gate_sig
    hidden = (gate_act * up_pre).astype(jnp.bfloat16)
    grad_gate_pre = (grad_hidden * up_pre * gate_sig * (1.0 + gate_pre * (1.0 - gate_sig))).astype(
        jnp.bfloat16
    )
    grad_up_pre = (grad_hidden * gate_act).astype(jnp.bfloat16)
    return hidden, grad_gate_pre, grad_up_pre


def block(index, size):
    return pl.ds(pl.multiple_of(index * size, size), size)


class Place:
    def __init__(self, nz, ny, nx):
        self.nz, self.ny, self.nx = nz, ny, nx
        fs, tp = lax.axis_index("fs"), lax.axis_index("tp")
        self.fs, self.tp = fs, tp
        self.z, self.y = fs // ny, fs % ny
        self.x, self.c = tp // CORES, tp % CORES

    def by_z(self, dz):
        return {"fs": ((self.z + dz) % self.nz) * self.ny + self.y, "tp": self.tp}

    def by_y(self, dy):
        return {"fs": self.z * self.ny + (self.y + dy) % self.ny, "tp": self.tp}

    def by_x(self, dx):
        return {"fs": self.fs, "tp": ((self.x + dx) % self.nx) * CORES + self.c}

    def by_core(self):
        return {"fs": self.fs, "tp": self.x * CORES + 1 - self.c}

    def by_tp(self, dt):
        return {"fs": self.fs, "tp": (self.tp + dt) % (self.nx * CORES)}


def meet(partners):
    barrier = pltpu.get_barrier_semaphore()
    for partner in partners:
        pl.semaphore_signal(barrier, inc=1, device_id=partner, device_id_type=MESH)
    pl.semaphore_wait(barrier, len(partners))


class Copies:
    def __init__(self, send_sem, recv_sem):
        self.send_sem, self.recv_sem, self.made = send_sem, recv_sem, []

    def start(self, source, target, device):
        at = len(self.made)
        copy = pltpu.make_async_remote_copy(
            src_ref=source, dst_ref=target, send_sem=self.send_sem.at[at],
            recv_sem=self.recv_sem.at[at], device_id=device, device_id_type=MESH,
        )
        copy.start()
        self.made.append(copy)
        return copy


def flip(value, mask, nz):
    bit = 1
    while bit < nz:
        if mask & bit:
            value = value + bit - 2 * bit * ((value // bit) % 2)
        bit *= 2
    return value


def far_first(nz):
    return sorted(range(1, nz), key=lambda d: -min(d, nz - d))


def low_bits(nz):
    return [1 << at for at in range(nz.bit_length() - 1)]


def fused_kernel(sizes, halves, x_ref, c_ref, *refs):
    nz, ny, nx = sizes
    me = Place(*sizes)
    w_refs, (r, out) = refs[:3], refs[3:5]
    xf, cf, wg, wd, pre, hid, gs, rg, sg, ps, rc, sx, rx, vz, sz, rz, send_sem, recv_sem = refs[5:]
    tokens, features = x_ref.shape
    depth, units = w_refs[0].shape[1], w_refs[0].shape[0] // nz
    part = units // halves
    rows = tokens * nz
    meet(
        [me.by_z(d) for d in range(1, nz)]
        + [me.by_y(d) for d in range(1, ny)]
        + [me.by_x(d) for d in range(1, nx)]
        + [me.by_core()]
    )
    copies = Copies(send_sem, recv_sem)
    wholes = (xf, cf)
    by_x, sent_z, w_sent, token_last = {}, {}, {}, []
    w_last = [[] for _ in range(halves)]
    bits = low_bits(nz)[::-1]
    order = far_first(nz)

    def chunk(mask):
        return block(flip(me.z, mask, nz), tokens)

    def spot(whole, mask, tp):
        return whole.at[chunk(mask), block(tp, features)]

    def w_source(at, h, dz):
        start = pl.multiple_of(((me.z + dz) % nz) * units + h * part, 16)
        return w_refs[at].at[pl.ds(start, part), :]

    def w_spot(at, h, dz):
        column = block(((me.z - dz + nz) % nz) * ny + me.y, depth)
        if at < 2:
            return wg.at[pl.ds((2 * h + at) * part, part), column]
        return wd.at[pl.ds(h * part, part), column]

    def held(mask):
        return (x_ref, c_ref) if mask == 0 else [spot(whole, mask, me.tp) for whole in wholes]

    def pass_z(bit, mask):
        there = {"fs": flip(me.z, bit, nz) * ny + me.y, "tp": me.tp}
        sent_z[bit, mask] = [
            copies.start(source, spot(whole, mask, me.tp), there)
            for source, whole in zip(held(mask), wholes)
        ]

    def pass_tp(mask):
        for dx in range(1, nx):
            by_x[mask, dx] = [
                copies.start(source, spot(whole, mask, me.tp), me.by_x(dx))
                for source, whole in zip(held(mask), wholes)
            ]
        for source, whole in zip(held(mask), wholes):
            token_last.append(copies.start(source, spot(whole, mask, me.tp), me.by_core()))

    def pass_core(mask):
        for dx in range(1, nx):
            tp = ((me.x - dx + nx) % nx) * CORES + me.c
            for copy, whole in zip(by_x[mask, dx], wholes):
                copy.wait_recv()
                here = spot(whole, mask, tp)
                token_last.append(copies.start(here, here, me.by_core()))

    def send_w(h, dz):
        w_sent[h, dz] = [
            copies.start(w_source(at, h, dz), w_spot(at, h, 0), me.by_z(dz)) for at in range(3)
        ]

    def own_w(h):
        for at in range(3):
            for dy in range(1, ny):
                copy = copies.start(w_source(at, h, 0), w_spot(at, h, 0), me.by_y(dy))
                w_last[h].append(copy)

    def relay_w(h, dz):
        for at, copy in enumerate(w_sent[h, dz]):
            copy.wait_recv()
            here = w_spot(at, h, dz)
            w_last[h] += [copies.start(here, here, me.by_y(dy)) for dy in range(1, ny)]

    for bit in bits:
        pass_z(bit, 0)
    pass_tp(0)
    send_w(0, order[0])
    own_w(0)
    for held_ref, whole in zip((x_ref, c_ref), wholes):
        whole[chunk(0), block(me.tp, features)] = held_ref[...]
    for h in range(halves):
        for at in range(3):
            start = pl.multiple_of(me.z * units + h * part, 16)
            w_spot(at, h, 0)[...] = w_refs[at][pl.ds(start, part), :]
    masks = [0]
    for at, bit in enumerate(bits):
        for mask in list(masks):
            for copy in sent_z[bit, mask]:
                copy.wait_recv()
            masks.append(mask + bit)
            for lower in bits[at + 1 :]:
                pass_z(lower, mask + bit)
            pass_tp(mask + bit)
        if at == 0:
            for dz in order[1:]:
                send_w(0, dz)
            for h in range(1, halves):
                for dz in order:
                    send_w(h, dz)
                own_w(h)
    for mask in masks:
        pass_core(mask)
    for dz in order:
        relay_w(0, dz)
    for copy in token_last:
        copy.wait_recv()

    tile = min(256, rows)

    def forward(h):
        pair = pl.ds(2 * h * part, 2 * part)
        single = pl.ds(h * part, part)

        def step(at, carry):
            some = block(at, tile)
            both = contract_cols(wg[pair, :], xf[some, :])
            grad_hidden = contract_cols(wd[single, :], cf[some, :])
            hidden, gate, up = pointwise(both[:part], both[part:], grad_hidden)
            hid[single, some] = hidden
            pre[pl.ds(2 * h * part, part), some] = gate
            pre[pl.ds((2 * h + 1) * part, part), some] = up
            return carry

        lax.fori_loop(0, rows // tile, step, 0)

    waiting = []

    def release():
        while waiting:
            sink, source, target, device = waiting.pop(0)
            sink.append(copies.start(source, target, device))

    def grads(h, dz, y):
        columns = block(((me.z + dz) % nz) * ny + y, depth)
        pair = jnp.dot(
            pre[pl.ds(2 * h * part, 2 * part), :], xf[:, columns], preferred_element_type=jnp.float32
        )
        single = jnp.dot(
            hid[pl.ds(h * part, part), :], cf[:, columns], preferred_element_type=jnp.float32
        )
        return pair, single

    to_y, final = {}, []

    def give(h, dz):
        pair, single = grads(h, dz, (me.y + 1) % ny)
        release()
        gs[h, dz, pl.ds(0, 2 * part), :] = pair.astype(gs.dtype)
        gs[h, dz, pl.ds(2 * part, part), :] = single.astype(gs.dtype)
        to_y[h, dz] = []
        waiting.append((to_y[h, dz], gs.at[h, dz], rg.at[h, dz], me.by_y(1)))

    def settle(h, dz):
        pair, single = grads(h, dz, me.y)
        release()
        to_y[h, dz][0].wait_recv()
        pair += rg[h, dz, pl.ds(0, 2 * part), :].astype(jnp.float32)
        single += rg[h, dz, pl.ds(2 * part, part), :].astype(jnp.float32)
        target = sg.at[h, dz] if dz else r.at[me.z, h]
        target[pl.ds(0, 2 * part), :] = pair.astype(sg.dtype)
        target[pl.ds(2 * part, part), :] = single.astype(sg.dtype)
        if dz:
            waiting.append((final, sg.at[h, dz], r.at[me.z, h], me.by_z(dz)))

    def partial(mask, tp):
        return contract_rows(pre[:, chunk(mask)], wg[:, block(tp, features)])

    back = sorted(masks, key=lambda mask: [mask & bit == 0 for bit in low_bits(nz)])
    to_core, to_x = {}, {}

    def give_core(mask):
        for x in range(nx):
            values = partial(mask, x * CORES + 1 - me.c)
            release()
            ps[mask, x] = values.astype(ps.dtype)
        to_core[mask] = []
        waiting.append((to_core[mask], ps.at[mask], rc.at[mask], me.by_core()))

    def give_x(mask):
        there = (me.x + 1) % nx
        values = partial(mask, there * CORES + me.c)
        release()
        to_core[mask][0].wait_recv()
        sx[mask] = (values + rc[mask, there].astype(jnp.float32)).astype(sx.dtype)
        to_x[mask] = []
        waiting.append((to_x[mask], sx.at[mask], rx.at[mask], me.by_x(1)))
        values = partial(mask, me.tp)
        release()
        vz[mask] = values + rc[mask, me.x].astype(jnp.float32)

    for h in range(halves):
        for copy in w_last[h]:
            copy.wait_recv()
        forward(h)
        for dz in order + [0]:
            give(h, dz)
        release()
        if h + 1 < halves:
            for dz in order:
                relay_w(h + 1, dz)
        else:
            for mask in back:
                give_core(mask)
            release()
        for dz in order + [0]:
            settle(h, dz)
        release()
    for mask in back:
        give_x(mask)
    release()
    for mask in back:
        to_x[mask][0].wait_recv()
        vz[mask] += rx[mask].astype(jnp.float32)
    left = list(masks)
    for bit in low_bits(nz):
        moving = [mask for mask in left if mask & bit]
        left = [mask for mask in left if not mask & bit]
        there = {"fs": flip(me.z, bit, nz) * ny + me.y, "tp": me.tp}
        came = {}
        for mask in moving:
            sz[mask] = vz[mask].astype(sz.dtype)
        for mask in moving:
            came[mask - bit] = copies.start(sz.at[mask], rz.at[mask], there)
        for mask in left:
            came[mask].wait_recv()
            vz[mask] += rz[mask + bit].astype(jnp.float32)
    out[...] = vz[0].astype(out.dtype)
    for copy in final:
        copy.wait_recv()
    for copy in copies.made:
        copy.wait_send()


def finish_kernel(r, g_ref, gate, up, down, g_out, gate_buf, up_buf, down_buf, sem):
    nz, halves, triple, depth = r.shape
    part = triple // 3
    outs = [pltpu.make_async_copy(g_ref, g_out, sem.at[0])]
    outs[0].start()
    for z in range(nz):
        for h in range(halves):
            spot = pl.ds((z * halves + h) * part, part)
            down_buf[spot, :] = r[z, h, pl.ds(2 * part, part), :].astype(jnp.float32)
    outs.append(pltpu.make_async_copy(down_buf, down, sem.at[1]))
    outs[-1].start()
    for at, (buf, target) in enumerate(((gate_buf, gate), (up_buf, up))):
        whole = jnp.concatenate(
            [r[z, h, pl.ds(at * part, part), :] for z in range(nz) for h in range(halves)], axis=0
        )
        buf[...] = whole.astype(jnp.float32).T
        outs.append(pltpu.make_async_copy(buf, target, sem.at[2 + at]))
        outs[-1].start()
    for copy in outs:
        copy.wait()


def split_plan(sizes, inputs, cotangent, gate_weight, up_weight, down_weight):
    nz, ny, nx = sizes
    tokens, features = inputs.shape
    depth, width = gate_weight.shape
    units, rows, model = width // nz, tokens * nz, depth * nz * ny
    halves = 2 if units % 32 == 0 else 1
    part = units // halves
    dma, half, full = pltpu.SemaphoreType.DMA, jnp.bfloat16, jnp.float32
    count = 2 * (nz - 1 + 2 * nz * nx) + 3 * halves * (nz - 1 + nz * (ny - 1))
    count += halves * (2 * nz - 1) + 2 * nz + nz - 1
    settled, grad_inputs = pl.pallas_call(
        functools.partial(fused_kernel, sizes, halves),
        out_shape=[
            jax.ShapeDtypeStruct((nz, halves, 3 * part, depth), half),
            jax.ShapeDtypeStruct((tokens, features), half),
        ],
        in_specs=[VMEM] * 5,
        out_specs=[VMEM, VMEM],
        scratch_shapes=[
            pltpu.VMEM((rows, model), half),
            pltpu.VMEM((rows, model), half),
            pltpu.VMEM((2 * units, model), half),
            pltpu.VMEM((units, model), half),
            pltpu.VMEM((2 * units, rows), half),
            pltpu.VMEM((units, rows), half),
            pltpu.VMEM((halves, nz, 3 * part, depth), half),
            pltpu.VMEM((halves, nz, 3 * part, depth), half),
            pltpu.VMEM((halves, nz, 3 * part, depth), half),
            pltpu.VMEM((nz, nx, tokens, features), half),
            pltpu.VMEM((nz, nx, tokens, features), half),
            pltpu.VMEM((nz, tokens, features), half),
            pltpu.VMEM((nz, tokens, features), half),
            pltpu.VMEM((nz, tokens, features), full),
            pltpu.VMEM((nz, tokens, features), half),
            pltpu.VMEM((nz, tokens, features), half),
            dma((count,)),
            dma((count,)),
        ],
        compiler_params=pltpu.CompilerParams(
            collective_id=0, has_side_effects=True, vmem_limit_bytes=60 * 2**20
        ),
    )(inputs, cotangent, gate_weight.T, up_weight.T, down_weight)
    gate, up, down, grad_inputs = pl.pallas_call(
        finish_kernel,
        out_shape=[
            jax.ShapeDtypeStruct((depth, width), full),
            jax.ShapeDtypeStruct((depth, width), full),
            jax.ShapeDtypeStruct((width, depth), full),
            jax.ShapeDtypeStruct((tokens, features), half),
        ],
        in_specs=[VMEM] * 2,
        out_specs=[ANY] * 4,
        scratch_shapes=[
            pltpu.VMEM((depth, width), full),
            pltpu.VMEM((depth, width), full),
            pltpu.VMEM((width, depth), full),
            dma((4,)),
        ],
    )(settled, grad_inputs)
    return grad_inputs, gate, up, down


def solution(mesh):
    n_fs, n_tp = mesh.shape["fs"], mesh.shape["tp"]
    nx = max(1, n_tp // CORES)
    ny = nx
    nz = n_fs // ny

    def per_device(inputs, cotangent, gate_weight, up_weight, down_weight):
        arrays = (inputs, cotangent, gate_weight, up_weight, down_weight)
        depth, width = gate_weight.shape
        fits = n_tp == nx * CORES and nz > 1 and ny > 1 and n_fs == nz * ny
        fits = fits and nz & (nz - 1) == 0 and nx == 2
        tiles = depth % 128 == 0 and inputs.shape[1] % 128 == 0 and inputs.shape[0] % 16 == 0
        if fits and tiles and width % (16 * nz) == 0:
            return split_plan((nz, ny, nx), *arrays)
        return gathered_plan(*arrays)

    return jax.shard_map(
        per_device,
        mesh=mesh,
        in_specs=(P("fs", "tp"), P("fs", "tp"), P("fs", "tp"), P("fs", "tp"), P("tp", "fs")),
        out_specs=(P("fs", "tp"), P("fs", "tp"), P("fs", "tp"), P("tp", "fs")),
        check_vma=False,
    )
```

```python
import functools

import jax
import jax.numpy as jnp
from jax import lax
from jax.experimental import pallas as pl
from jax.experimental.pallas import tpu as pltpu
from jax.sharding import PartitionSpec as P

MESH = pl.DeviceIdType.MESH
ANY = pl.BlockSpec(memory_space=pl.ANY)
VMEM = pl.BlockSpec(memory_space=pltpu.VMEM)
CORES = 2


def contract_rows(left, right):
    return lax.dot_general(
        left, right, (((0,), (0,)), ((), ())), preferred_element_type=jnp.float32
    )


def contract_cols(left, right):
    return lax.dot_general(
        left, right, (((1,), (1,)), ((), ())), preferred_element_type=jnp.float32
    )


def gathered_plan(inputs, cotangent, gate_weight, up_weight, down_weight):
    whole_inputs = lax.all_gather(inputs, "tp", axis=1, tiled=True)
    whole_cotangent = lax.all_gather(cotangent, "tp", axis=1, tiled=True)
    gate_whole = lax.all_gather(gate_weight, "fs", axis=0, tiled=True)
    up_whole = lax.all_gather(up_weight, "fs", axis=0, tiled=True)
    down_whole = lax.all_gather(down_weight, "fs", axis=1, tiled=True)
    gate_pre = jnp.dot(whole_inputs, gate_whole, preferred_element_type=jnp.float32)
    up_pre = jnp.dot(whole_inputs, up_whole, preferred_element_type=jnp.float32)
    grad_hidden = contract_cols(whole_cotangent, down_whole)
    hidden, grad_gate_pre, grad_up_pre = pointwise(gate_pre, up_pre, grad_hidden)
    pre_grads = jnp.concatenate([grad_gate_pre, grad_up_pre], axis=1)
    width = gate_weight.shape[1]
    partial_sum = contract_cols(grad_gate_pre, gate_whole) + contract_cols(grad_up_pre, up_whole)

    def scattered(values, axis, dim):
        return lax.psum_scatter(
            values.astype(jnp.bfloat16), axis, scatter_dimension=dim, tiled=True
        )

    grad_inputs = scattered(partial_sum, "tp", 1)
    expand = scattered(contract_rows(whole_inputs, pre_grads), "fs", 0).astype(jnp.float32)
    down = scattered(contract_rows(whole_cotangent, hidden), "fs", 0).astype(jnp.float32)
    return (grad_inputs, expand[:, :width], expand[:, width:], down.T)


def pointwise(gate_pre, up_pre, grad_hidden):
    gate_sig = jax.nn.sigmoid(gate_pre)
    gate_act = gate_pre * gate_sig
    hidden = (gate_act * up_pre).astype(jnp.bfloat16)
    grad_gate_pre = (grad_hidden * up_pre * gate_sig * (1.0 + gate_pre * (1.0 - gate_sig))).astype(
        jnp.bfloat16
    )
    grad_up_pre = (grad_hidden * gate_act).astype(jnp.bfloat16)
    return hidden, grad_gate_pre, grad_up_pre


def block(index, size):
    return pl.ds(pl.multiple_of(index * size, size), size)


class Place:
    def __init__(self, nz, ny, nx):
        self.nz, self.ny, self.nx = nz, ny, nx
        fs, tp = lax.axis_index("fs"), lax.axis_index("tp")
        self.fs, self.tp = fs, tp
        self.z, self.y = fs // ny, fs % ny
        self.x, self.c = tp // CORES, tp % CORES

    def by_z(self, dz):
        return {"fs": ((self.z + dz) % self.nz) * self.ny + self.y, "tp": self.tp}

    def by_y(self, dy):
        return {"fs": self.z * self.ny + (self.y + dy) % self.ny, "tp": self.tp}

    def by_x(self, dx):
        return {"fs": self.fs, "tp": ((self.x + dx) % self.nx) * CORES + self.c}

    def by_core(self):
        return {"fs": self.fs, "tp": self.x * CORES + 1 - self.c}

    def by_tp(self, dt):
        return {"fs": self.fs, "tp": (self.tp + dt) % (self.nx * CORES)}


def meet(partners):
    barrier = pltpu.get_barrier_semaphore()
    for partner in partners:
        pl.semaphore_signal(barrier, inc=1, device_id=partner, device_id_type=MESH)
    pl.semaphore_wait(barrier, len(partners))


class Copies:
    def __init__(self, send_sem, recv_sem):
        self.send_sem, self.recv_sem, self.made = send_sem, recv_sem, []

    def start(self, source, target, device):
        at = len(self.made)
        copy = pltpu.make_async_remote_copy(
            src_ref=source, dst_ref=target, send_sem=self.send_sem.at[at],
            recv_sem=self.recv_sem.at[at], device_id=device, device_id_type=MESH,
        )
        copy.start()
        self.made.append(copy)
        return copy


def flip(value, mask, nz):
    bit = 1
    while bit < nz:
        if mask & bit:
            value = value + bit - 2 * bit * ((value // bit) % 2)
        bit *= 2
    return value


def far_first(nz):
    return sorted(range(1, nz), key=lambda d: -min(d, nz - d))


def low_bits(nz):
    return [1 << at for at in range(nz.bit_length() - 1)]


def fused_kernel(sizes, halves, *refs):
    nz, ny, nx = sizes
    me = Place(*sizes)
    ins, (r, out), (raw, turned, xf, cf, wg, wd) = refs[:5], refs[5:7], refs[7:13]
    pre, hid, gs, rg, sg, ps, rc, sx, rx, vz, sz, rz, send_sem, recv_sem, own_sem = refs[13:]
    tokens, features = ins[0].shape
    depth, units = ins[2].shape[0], ins[2].shape[1] // nz
    part = units // halves
    rows = tokens * nz
    scope = jax.named_scope
    copies = Copies(send_sem, recv_sem)
    wholes = (xf, cf)
    by_x, sent_z, w_sent, token_last = {}, {}, {}, []
    w_last = [[] for _ in range(halves)]
    bits = low_bits(nz)
    order = sorted(range(1, nz), key=lambda mask: (mask & -mask == 1, mask))
    order = sorted(order, key=lambda mask: mask < nz // 2)

    def chunk(mask):
        return block(flip(me.z, mask, nz), tokens)

    def by_flip(mask):
        return {"fs": flip(me.z, mask, nz) * ny + me.y, "tp": me.tp}

    def spot(at, mask, tp):
        return wholes[at].at[chunk(mask), block(tp, features)]

    def w_source(at, h, mask):
        start = pl.multiple_of(flip(me.z, mask, nz) * units + h * part, 16)
        return turned.at[at, pl.ds(start, part), :]

    def w_spot(at, h, mask):
        column = block(flip(me.z, mask, nz) * ny + me.y, depth)
        if at < 2:
            return wg.at[pl.ds((2 * h + at) * part, part), column]
        return wd.at[pl.ds(h * part, part), column]

    fetch = [pltpu.make_async_copy(ins[at], spot(at, 0, me.tp), own_sem.at[at]) for at in range(2)]
    fetch += [pltpu.make_async_copy(ins[2 + at], raw.at[at], own_sem.at[2 + at]) for at in range(2)]
    fetch.append(pltpu.make_async_copy(ins[4], turned.at[2], own_sem.at[4]))
    for copy in fetch:
        copy.start()
    with scope("meet"):
        meet(
            [me.by_z(d) for d in range(1, nz)]
            + [me.by_y(d) for d in range(1, ny)]
            + [me.by_x(d) for d in range(1, nx)]
            + [me.by_core()]
        )

    def pass_z(bit, mask, at):
        here = spot(at, mask, me.tp)
        sent_z[bit, mask, at] = copies.start(here, here, by_flip(bit))

    def pass_tp(mask, at):
        here = spot(at, mask, me.tp)
        for dx in range(1, nx):
            by_x[mask, dx, at] = copies.start(here, here, me.by_x(dx))
        token_last.append(copies.start(here, here, me.by_core()))

    def pass_core(mask, at):
        for dx in range(1, nx):
            tp = ((me.x - dx + nx) % nx) * CORES + me.c
            by_x[mask, dx, at].wait_recv()
            here = spot(at, mask, tp)
            token_last.append(copies.start(here, here, me.by_core()))

    def take_tokens(bit, mask, at):
        sent_z[bit, mask, at].wait_recv()
        for lower in bits:
            if lower < bit and mask % (2 * bit) == 0:
                pass_z(lower, mask + bit, at)
        pass_tp(mask + bit, at)

    def send_w(h, mask):
        w_sent[h, mask] = [
            copies.start(w_source(at, h, mask), w_spot(at, h, 0), by_flip(mask))
            for at in range(3)
        ]

    def own_w(h, at):
        for dy in range(1, ny):
            w_last[h].append(copies.start(w_source(at, h, 0), w_spot(at, h, 0), me.by_y(dy)))

    def relay_w(h, mask):
        for at, copy in enumerate(w_sent[h, mask]):
            copy.wait_recv()
            here = w_spot(at, h, mask)
            w_last[h] += [copies.start(here, here, me.by_y(dy)) for dy in range(1, ny)]

    def do(what, *key):
        with scope(f"{what.__name__}#" + "#".join(str(k) for k in key)):
            what(*key)

    for at in range(2):
        fetch[at].wait()
        for bit in bits:
            pass_z(bit, 0, at)
        pass_tp(0, at)
    fetch[4].wait()
    for h in range(halves):
        own_w(h, 2)
    with scope("turn"):
        for at in range(2):
            fetch[2 + at].wait()
            for start in range(0, units * nz, 128):
                some = pl.ds(start, 128)
                turned[at, some, :] = raw[at, :, some].T
    for h in range(halves):
        for at in range(2):
            own_w(h, at)
    send_w(0, order[0])
    for h in range(halves):
        for at in range(3):
            start = pl.multiple_of(me.z * units + h * part, 16)
            w_spot(at, h, 0)[...] = turned[at, pl.ds(start, part), :]
    later = []
    for mask in range(1, nz):
        later += [(bit, mask) for bit in bits if bit < (mask & -mask)]
    cores = [(0, 0), (0, 1)]
    for at in range(2):
        for bit in bits:
            do(take_tokens, bit, 0, at)
            cores.append((bit, at))
        for key in cores[:2]:
            do(pass_core, *key)
        cores = cores[2:]
    for mask in order[1:]:
        send_w(0, mask)
    for key in cores[:1]:
        do(pass_core, *key)
    cores = cores[1:]
    for bit, mask in later:
        do(take_tokens, bit, mask, 0)
        cores.append((mask + bit, 0))
    do(relay_w, 0, order[0])
    for bit, mask in later:
        do(take_tokens, bit, mask, 1)
        cores.append((mask + bit, 1))
    for h in range(1, halves):
        for mask in order:
            send_w(h, mask)
    for key in cores[:-2]:
        do(pass_core, *key)
    for mask in order[1:]:
        do(relay_w, 0, mask)
    for key in cores[-2:]:
        do(pass_core, *key)
    with scope("wait_tokens"):
        for copy in token_last:
            copy.wait_recv()

    tile = min(256, rows)

    def forward(h):
        pair = pl.ds(2 * h * part, 2 * part)
        single = pl.ds(h * part, part)

        def step(at, carry):
            some = block(at, tile)
            both = contract_cols(wg[pair, :], xf[some, :])
            grad_hidden = contract_cols(wd[single, :], cf[some, :])
            hidden, gate, up = pointwise(both[:part], both[part:], grad_hidden)
            hid[single, some] = hidden
            pre[pl.ds(2 * h * part, part), some] = gate
            pre[pl.ds((2 * h + 1) * part, part), some] = up
            return carry

        lax.fori_loop(0, rows // tile, step, 0)

    waiting = []

    def release():
        while waiting:
            sink, source, target, device = waiting.pop(0)
            sink.append(copies.start(source, target, device))

    def grads(h, mask, y):
        columns = block(flip(me.z, mask, nz) * ny + y, depth)
        pair = jnp.dot(
            pre[pl.ds(2 * h * part, 2 * part), :], xf[:, columns], preferred_element_type=jnp.float32
        )
        single = jnp.dot(
            hid[pl.ds(h * part, part), :], cf[:, columns], preferred_element_type=jnp.float32
        )
        return pair, single

    to_y, final = {}, []

    def give(h, mask):
        pair, single = grads(h, mask, (me.y + 1) % ny)
        release()
        gs[h, mask, pl.ds(0, 2 * part), :] = pair.astype(gs.dtype)
        gs[h, mask, pl.ds(2 * part, part), :] = single.astype(gs.dtype)
        to_y[h, mask] = []
        waiting.append((to_y[h, mask], gs.at[h, mask], rg.at[h, mask], me.by_y(1)))

    def settle(h, mask):
        pair, single = grads(h, mask, me.y)
        release()
        with scope("wait_y"):
            to_y[h, mask][0].wait_recv()
        pair += rg[h, mask, pl.ds(0, 2 * part), :].astype(jnp.float32)
        single += rg[h, mask, pl.ds(2 * part, part), :].astype(jnp.float32)
        sg[h, mask, pl.ds(0, 2 * part), :] = pair.astype(sg.dtype)
        sg[h, mask, pl.ds(2 * part, part), :] = single.astype(sg.dtype)
        if mask:
            waiting.append((final, sg.at[h, mask], r.at[me.z, h], by_flip(mask)))

    def partial(mask, tp):
        return contract_rows(pre[:, chunk(mask)], wg[:, block(tp, features)])

    back = sorted(range(nz), key=lambda mask: [mask & bit == 0 for bit in bits])
    to_core, to_x = {}, {}

    def give_core(mask):
        for x in range(nx):
            values = partial(mask, x * CORES + 1 - me.c)
            release()
            ps[mask, x] = values.astype(ps.dtype)
        to_core[mask] = []
        waiting.append((to_core[mask], ps.at[mask], rc.at[mask], me.by_core()))

    def give_x(mask):
        there = (me.x + 1) % nx
        values = partial(mask, there * CORES + me.c)
        release()
        to_core[mask][0].wait_recv()
        sx[mask] = (values + rc[mask, there].astype(jnp.float32)).astype(sx.dtype)
        to_x[mask] = []
        waiting.append((to_x[mask], sx.at[mask], rx.at[mask], me.by_x(1)))
        values = partial(mask, me.tp)
        release()
        vz[mask] = values + rc[mask, me.x].astype(jnp.float32)

    def ready(h):
        release()
        with scope(f"wait_w#h={h}"):
            for copy in w_last[h]:
                copy.wait_recv()
        with scope(f"forward#h={h}"):
            forward(h)

    def take_x(mask):
        release()
        to_x[mask][0].wait_recv()
        vz[mask] += rx[mask].astype(jnp.float32)

    came = {}

    def send_z(bit, mask):
        sz[mask] = vz[mask].astype(sz.dtype)
        came[bit, mask - bit] = []
        waiting.append((came[bit, mask - bit], sz.at[mask], rz.at[mask], by_flip(bit)))

    def take_z(bit, mask):
        release()
        came[bit, mask][0].wait_recv()
        vz[mask] += rz[mask + bit].astype(jnp.float32)

    last = halves - 1
    for h in range(last):
        ready(h)
        for at, mask in enumerate(order):
            do(give, h, mask)
            release()
            do(relay_w, h + 1, mask)
            if at:
                do(settle, h, order[at - 1])
    ready(last)
    for mask in order:
        do(give, last, mask)
    for mask in back:
        do(give_core, mask)
    for mask in back:
        do(give_x, mask)
    steps = [(settle, h, order[-1]) for h in range(last)]
    steps += [(settle, last, mask) for mask in order]
    for h in range(halves):
        steps += [(give, h, 0)]
    steps += [(settle, h, 0) for h in range(halves)]

    def step(count=1):
        for _ in range(min(count, len(steps))):
            do(*steps.pop(0))
        release()

    step(2)
    left = list(back)
    for mask in back:
        do(take_x, mask)
        if mask & 1:
            do(send_z, 1, mask)
        step()
    left = [mask for mask in back if not mask & 1]
    for at, bit in enumerate(bits):
        higher = bits[at + 1 :]
        for mask in left:
            do(take_z, bit, mask)
            if higher and mask & higher[0]:
                do(send_z, higher[0], mask)
            step()
        left = [mask for mask in left if not (higher and mask & higher[0])]
    step(len(steps))
    local = [
        pltpu.make_async_copy(sg.at[h, 0], r.at[me.z, h], own_sem.at[h]) for h in range(halves)
    ]
    for copy in local:
        copy.start()
    out[...] = vz[0].astype(out.dtype)
    with scope("wait_final"):
        for copy in final:
            copy.wait_recv()
    with scope("wait_sends"):
        for copy in copies.made:
            copy.wait_send()
        for copy in local:
            copy.wait()


def finish_kernel(r, g_ref, gate, up, down, g_out, gate_buf, up_buf, down_buf, sem):
    nz, halves, triple, depth = r.shape
    part = triple // 3
    outs = [pltpu.make_async_copy(g_ref, g_out, sem.at[0])]
    outs[0].start()
    for z in range(nz):
        for h in range(halves):
            spot = pl.ds((z * halves + h) * part, part)
            down_buf[spot, :] = r[z, h, pl.ds(2 * part, part), :].astype(jnp.float32)
    outs.append(pltpu.make_async_copy(down_buf, down, sem.at[1]))
    outs[-1].start()
    for at, (buf, target) in enumerate(((gate_buf, gate), (up_buf, up))):
        whole = jnp.concatenate(
            [r[z, h, pl.ds(at * part, part), :] for z in range(nz) for h in range(halves)], axis=0
        )
        buf[...] = whole.astype(jnp.float32).T
        outs.append(pltpu.make_async_copy(buf, target, sem.at[2 + at]))
        outs[-1].start()
    for copy in outs:
        copy.wait()


def split_plan(sizes, inputs, cotangent, gate_weight, up_weight, down_weight):
    nz, ny, nx = sizes
    tokens, features = inputs.shape
    depth, width = gate_weight.shape
    units, rows, model = width // nz, tokens * nz, depth * nz * ny
    halves = 2 if units % 32 == 0 else 1
    part = units // halves
    dma, half, full = pltpu.SemaphoreType.DMA, jnp.bfloat16, jnp.float32
    count = 2 * (nz - 1 + 2 * nz * nx) + 3 * halves * (nz - 1 + nz * (ny - 1))
    count += halves * (2 * nz - 1) + 2 * nz + nz - 1
    settled, grad_inputs = pl.pallas_call(
        functools.partial(fused_kernel, sizes, halves),
        out_shape=[
            jax.ShapeDtypeStruct((nz, halves, 3 * part, depth), half),
            jax.ShapeDtypeStruct((tokens, features), half),
        ],
        in_specs=[ANY] * 5,
        out_specs=[ANY, VMEM],
        scratch_shapes=[
            pltpu.VMEM((2, depth, width), half),
            pltpu.VMEM((3, width, depth), half),
            pltpu.VMEM((rows, model), half),
            pltpu.VMEM((rows, model), half),
            pltpu.VMEM((2 * units, model), half),
            pltpu.VMEM((units, model), half),
            pltpu.VMEM((2 * units, rows), half),
            pltpu.VMEM((units, rows), half),
            pltpu.VMEM((halves, nz, 3 * part, depth), half),
            pltpu.VMEM((halves, nz, 3 * part, depth), half),
            pltpu.VMEM((halves, nz, 3 * part, depth), half),
            pltpu.VMEM((nz, nx, tokens, features), half),
            pltpu.VMEM((nz, nx, tokens, features), half),
            pltpu.VMEM((nz, tokens, features), half),
            pltpu.VMEM((nz, tokens, features), half),
            pltpu.VMEM((nz, tokens, features), full),
            pltpu.VMEM((nz, tokens, features), half),
            pltpu.VMEM((nz, tokens, features), half),
            dma((count,)),
            dma((count,)),
            dma((5,)),
        ],
        compiler_params=pltpu.CompilerParams(
            collective_id=0, has_side_effects=True, vmem_limit_bytes=60 * 2**20
        ),
    )(inputs, cotangent, gate_weight, up_weight, down_weight)
    gate, up, down, grad_inputs = pl.pallas_call(
        finish_kernel,
        out_shape=[
            jax.ShapeDtypeStruct((depth, width), full),
            jax.ShapeDtypeStruct((depth, width), full),
            jax.ShapeDtypeStruct((width, depth), full),
            jax.ShapeDtypeStruct((tokens, features), half),
        ],
        in_specs=[VMEM] * 2,
        out_specs=[ANY] * 4,
        scratch_shapes=[
            pltpu.VMEM((depth, width), full),
            pltpu.VMEM((depth, width), full),
            pltpu.VMEM((width, depth), full),
            dma((4,)),
        ],
    )(settled, grad_inputs)
    return grad_inputs, gate, up, down


def solution(mesh):
    n_fs, n_tp = mesh.shape["fs"], mesh.shape["tp"]
    nx = max(1, n_tp // CORES)
    ny = nx
    nz = n_fs // ny

    def per_device(inputs, cotangent, gate_weight, up_weight, down_weight):
        arrays = (inputs, cotangent, gate_weight, up_weight, down_weight)
        depth, width = gate_weight.shape
        fits = n_tp == nx * CORES and nz > 1 and ny > 1 and n_fs == nz * ny
        fits = fits and nz & (nz - 1) == 0 and nx == 2
        tiles = depth % 128 == 0 and inputs.shape[1] % 128 == 0 and inputs.shape[0] % 16 == 0
        if fits and tiles and width % (16 * nz) == 0:
            return split_plan((nz, ny, nx), *arrays)
        return gathered_plan(*arrays)

    return jax.shard_map(
        per_device,
        mesh=mesh,
        in_specs=(P("fs", "tp"), P("fs", "tp"), P("fs", "tp"), P("fs", "tp"), P("tp", "fs")),
        out_specs=(P("fs", "tp"), P("fs", "tp"), P("fs", "tp"), P("tp", "fs")),
        check_vma=False,
    )
```
